32 devices in a mesh: ep: 8 (over z, y), tp: 4 (over x, core).
Axes of the slice: x: 2, y: 2, z: 4, core: 2. Of those that a mesh axis runs over, the one named last changes fastest.
Arguments:
- queries: bfloat16 [2048, 8, 128], P('ep', 'tp'), may hold values from -15 to 15
- keys: bfloat16 [2048, 4, 128], P('ep', 'tp'), may hold values from -6 to 6
- values: bfloat16 [2048, 4, 128], P('ep', 'tp'), may hold values from -6 to 6
- key_bias: bfloat16 [2048, 8], P('ep', 'tp'), may hold values from -20 to 2
- out_weight: bfloat16 [1024, 2048], P('tp'), may hold values from -0.1875 to 0.1875
- tokens_b: bfloat16 [4096, 2048], P(('ep', 'tp')), may hold values from -6 to 6
- moe_gain: bfloat16 [2048], replicated, may hold values from 0.099609375 to 1.8984375
- gate_weight: bfloat16 [8, 2048, 2048], P('ep', None, 'tp'), may hold values from -0.125 to 0.125
- up_weight: bfloat16 [8, 2048, 2048], P('ep', None, 'tp'), may hold values from -0.125 to 0.125
- down_weight: bfloat16 [8, 2048, 2048], P('ep', 'tp'), may hold values from -0.125 to 0.125
- routes: int32 [4096, 2], P(('ep', 'tp')), may hold values from 0 to 7, all different within a row; in each aligned block of 128 rows (0 to 127, 128 to 255, ...) at most 48 rows name the same one
- route_weights: float32 [4096, 2], P(('ep', 'tp')), may hold values from 0.2 to 1
Outputs:
- mixed: bfloat16 [2048, 2048], P(('ep', 'tp'))
- moe_out: bfloat16 [4096, 2048], P(('ep', 'tp'))
The draws below stay inside these ranges and needn't reach their ends.
Inputs may be any that keep to these rules, and one draw needn't show every extreme that they name: `routes`: each row names 2 different experts. In each aligned block of 128 rows (the rows of one device) no expert is named by more than 48 rows, and in some block one expert is named by exactly 48 rows.
All inputs are finite; a program needn't handle non-finite values.
Results may differ from the reference program's by a relative error of at most 0.012.
Values may be sent and summed in bfloat16 or wider, within the bound.
No kernel may reach another device: no remote copies, remote signals or barrier semaphores. Data moves between devices by JAX's collectives and lax.ppermute only.
A program may use at most 128 MiB of HBM per device.

```python
import math
import jax
import jax.numpy as jnp
import numpy as np
from jax import lax

D = 2048
HEADS = 8
KV_HEADS = 4
DH = 128
FF = 2048
TOP = 2
TOK_A = 256
TOK_B = 128
EXPERTS = 8
CAP = 48
GROUPS = 4
ATTENTION_TOKENS = 2048
TOKENS_B = 4096


def draw_key_bias(key, part):
    chooser = jax.random.uniform(jax.random.fold_in(key, 11), (HEADS,))
    slow_heads = chooser < 0.5
    slow_level = -jnp.log(ATTENTION_TOKENS * 23.0)
    levels = jnp.where(slow_heads, slow_level, -6.5)
    block_shift = jax.random.uniform(jax.random.fold_in(key, 12), (ATTENTION_TOKENS // TOK_A,), minval=-0.8, maxval=0.8)
    roughness = jax.random.uniform(jax.random.fold_in(key, 13), (ATTENTION_TOKENS, HEADS), minval=-1.0, maxval=1.0)
    release_point = jax.random.randint(jax.random.fold_in(key, 14), (3,), 0, ATTENTION_TOKENS)
    sequence_places = jnp.arange(ATTENTION_TOKENS)
    releasing_now = jnp.any(sequence_places[:, None] == release_point[None, :], axis=1)
    steady = levels[None, :] + jnp.repeat(block_shift, TOK_A)[:, None]
    drawn = jnp.where(releasing_now[:, None], -1.5, steady) + roughness
    return drawn.astype(jnp.float32).astype(jnp.bfloat16)


def shard_levels(rng, extent, split, smallest, largest):
    def one(dim, shards_of):
        draws = jax.random.uniform(jax.random.fold_in(jax.random.fold_in(rng, 6), dim), (shards_of,), jnp.float32, smallest / len(split), largest / len(split))
        return jnp.repeat(jnp.exp(draws), extent[dim] // shards_of).reshape((-1,) + (1,) * (len(extent) - dim - 1))

    factor_of = one(*split[0])
    for cut in split[1:]:
        factor_of = factor_of * one(*cut)
    return factor_of


def deal_out(stream_key, own, number, rows, number_of, top, limit, lean):
    ranking = jax.random.permutation(stream_key, number_of)
    crowded, ordinary = portions_of(number_of, rows * top, limit, lean, True), portions_of(number_of, rows * top, limit, lean, False)
    places = jnp.arange(number_of)

    def named(sizes, turn):
        used = int((sizes > 0).sum())
        fixed = max(1, used // 4)
        shifted = fixed + (places - fixed + turn * (used - fixed)) % max(1, number_of - fixed)
        return jnp.zeros((number_of,), jnp.int32).at[ranking[jnp.where(places < fixed, places, shifted)]].set(jnp.asarray(sizes, jnp.int32))

    sizes = jnp.where(number % 4 == 0, named(crowded, number // 4), named(ordinary, number - number // 4 - 1))
    mixed = jax.random.permutation(jax.random.fold_in(own, 3), number_of)
    donor, receiver = mixed[0:number_of // 2 * 2:2], mixed[1:number_of // 2 * 2:2]
    slack = jnp.minimum(sizes[donor] - 1, limit - sizes[receiver]) // 2
    slack = jnp.where((donor == ranking[0]) | (receiver == ranking[0]) | (sizes[receiver] == 0), 0, jnp.maximum(slack, 0))
    shifted = jax.random.randint(jax.random.fold_in(own, 4), (number_of // 2,), 0, 1 << 20) % (slack + 1)
    sizes = sizes.at[donor].add(-shifted).at[receiver].add(shifted)
    items = jnp.searchsorted(jnp.cumsum(sizes), jnp.arange(rows * top), side="right").astype(jnp.int32)
    table = items.reshape(top, rows).T
    table = table[jax.random.permutation(jax.random.fold_in(own, 1), rows)]
    turn = jax.random.randint(jax.random.fold_in(own, 2), (rows, 1), 0, top)
    return jnp.take_along_axis(table, (jnp.arange(top)[None, :] + turn) % top, axis=1)


def portions_of(count, total, most, skew, full):
    weights = [(1 << 20) // math.isqrt(standing ** skew) + 1 for standing in range(1, count + 1)]
    largest = most if full else min(most, max(-(-total // count), total * weights[0] // sum(weights)))
    least = 1 if total - largest >= count - 1 else 0
    given, spare = [largest] + [least] * (count - 1), total - largest - least * (count - 1)
    while spare > 0:
        candidates = [i for i in range(1, count) if given[i] < largest] or [i for i in range(1, count) if given[i] < most]
        mass, left = sum([weights[i] for i in candidates]), spare
        for i in candidates:
            more = min(most - given[i], max(1, left * weights[i] // mass), spare)
            given[i] = given[i] + more
            spare = spare - more
    return np.array(given)


def bell_draw(own_key, dims, width, bound, split=(), held_as=jnp.bfloat16):
    entries = width * jax.random.normal(own_key, dims, jnp.float32)
    if split:
        entries = entries * shard_levels(own_key, dims, split, -0.22, 0.18)
    return jnp.clip(entries, -bound, bound).astype(held_as)


def setup_inputs(seed: int = 0) -> dict:
    streams_of = jax.random.split(jax.random.key(seed), 13)
    queries = bell_draw(streams_of[0], (ATTENTION_TOKENS, HEADS, DH), 2.5, 15.0, ((0, 8), (1, 4)))
    keys = bell_draw(streams_of[1], (ATTENTION_TOKENS, KV_HEADS, DH), 1.0, 6.0, ((0, 8), (1, 4)))
    values = bell_draw(streams_of[2], (ATTENTION_TOKENS, KV_HEADS, DH), 1.0, 6.0, ((0, 8), (1, 4)))
    key_bias = draw_key_bias(jax.random.fold_in(streams_of[12], 71), 0)
    out_weight = bell_draw(streams_of[4], (HEADS * DH, D), (HEADS * DH) ** -0.5, 0.1875, ((0, 4),))
    tokens_b = bell_draw(streams_of[5], (TOKENS_B, D), 1.0, 6.0, ((0, 32),))
    moe_gain = jnp.clip(1.0 + 0.18 * jax.random.normal(streams_of[6], (D,), jnp.float32), 0.099609375, 1.8984375).astype(jnp.bfloat16)
    gate_weight = bell_draw(streams_of[7], (EXPERTS, D, FF), D ** -0.5, 0.125, ((0, 8), (2, 4)))
    up_weight = bell_draw(streams_of[8], (EXPERTS, D, FF), D ** -0.5, 0.125, ((0, 8), (2, 4)))
    down_weight = bell_draw(streams_of[9], (EXPERTS, FF, D), FF ** -0.5, 0.125, ((0, 8), (1, 4)))
    routes_keys = jax.random.split(jax.random.fold_in(streams_of[10], 1), TOKENS_B // TOK_B)
    routes_turns = jax.random.permutation(jax.random.fold_in(streams_of[10], 3), TOKENS_B // TOK_B)
    routes = jax.vmap(lambda own, number: deal_out(jax.random.fold_in(streams_of[10], 2), own, number, TOK_B, EXPERTS, TOP, CAP, 2))(routes_keys, routes_turns).reshape((TOKENS_B, TOP))
    route_weights = jnp.clip(0.2 + 0.8 * jax.random.uniform(streams_of[11], (TOKENS_B, TOP), jnp.float32) ** shard_levels(streams_of[11], (TOKENS_B, TOP), ((0, 32),), -0.2, 0.2), 0.2, 1.0)
    return dict(queries=queries, keys=keys, values=values, key_bias=key_bias, out_weight=out_weight, tokens_b=tokens_b, moe_gain=moe_gain, gate_weight=gate_weight, up_weight=up_weight, down_weight=down_weight, routes=routes, route_weights=route_weights)


def to_bf_and_back(partial_sum):
    return lax.optimization_barrier(partial_sum.astype(jnp.bfloat16)).astype(jnp.float32)

def stick_rows(query_block, first_pos, keys_all, values_all, bias_all):
    block_len = query_block.shape[0]
    group_size = HEADS // KV_HEADS
    query_f = query_block.astype(jnp.float32).reshape(block_len, KV_HEADS, group_size, DH)
    scores = jnp.einsum('rkgd,skd->kgrs', query_f, keys_all) / math.sqrt(DH)
    scores = scores + bias_all[:, :, None, :]
    query_pos = first_pos + jnp.arange(block_len, dtype=jnp.int32)
    key_pos = jnp.arange(ATTENTION_TOKENS, dtype=jnp.int32)
    earlier = key_pos[None, :] < query_pos[:, None]
    log_keep = jnp.where(earlier, jax.nn.log_sigmoid(-scores), 0.0)
    after = lax.cumsum(log_keep, axis=3, reverse=True) - log_keep
    weights = jnp.where(earlier, jnp.exp(jax.nn.log_sigmoid(scores) + after), 0.0).astype(jnp.bfloat16)
    attended = jnp.einsum('kgrs,skd->rkgd', weights.astype(jnp.float32), values_all)
    return attended.reshape(block_len, HEADS * DH).astype(jnp.bfloat16)

def reference(queries, keys, values, key_bias, out_weight, tokens_b, moe_gain, gate_weight, up_weight, down_weight, routes, route_weights):
    group_size = HEADS // KV_HEADS
    keys_all = keys.astype(jnp.float32)
    values_all = values.astype(jnp.float32)
    bias_all = jnp.transpose(key_bias.astype(jnp.float32).reshape(ATTENTION_TOKENS, KV_HEADS, group_size), (1, 2, 0))
    block_len = math.gcd(ATTENTION_TOKENS, 512)
    block_total = ATTENTION_TOKENS // block_len
    query_blocks = queries.reshape(block_total, block_len, HEADS, DH)
    first_positions = (jnp.arange(block_total) * block_len).astype(jnp.int32)

    def one_block(operands):
        return stick_rows(operands[0], operands[1], keys_all, values_all, bias_all)
    attended = lax.map(one_block, (query_blocks, first_positions)).reshape(ATTENTION_TOKENS, HEADS * DH)
    head_width = HEADS * DH // GROUPS
    mixed_sum = jnp.zeros((ATTENTION_TOKENS, D), jnp.float32)
    for group_no in range(GROUPS):
        lower = group_no * head_width
        partial_sum = jnp.dot(attended[:, lower:lower + head_width], out_weight[lower:lower + head_width], preferred_element_type=jnp.float32)
        mixed_sum = mixed_sum + to_bf_and_back(partial_sum)
    mixed = mixed_sum.astype(jnp.bfloat16)
    tokens_f = tokens_b.astype(jnp.float32)
    normed = (tokens_f * lax.rsqrt(lax.optimization_barrier(jnp.mean(tokens_f * tokens_f, axis=1, keepdims=True)) + 1e-06) * moe_gain.astype(jnp.float32)).astype(jnp.bfloat16)
    block_count = TOKENS_B // TOK_B
    flattened_expert_list = routes.reshape(block_count, TOK_B * TOP)
    onehot = (flattened_expert_list[:, :, None] == jnp.arange(EXPERTS, dtype=jnp.int32)[None, None, :]).astype(jnp.int32)
    earlier_count = jnp.cumsum(onehot, axis=1) - onehot
    slot_index = lax.optimization_barrier(jnp.sum(earlier_count * onehot, axis=2))
    block_ids = jnp.arange(block_count, dtype=jnp.int32)[:, None]
    place = (block_ids * CAP + slot_index).astype(jnp.int32)
    token_ids = (block_ids * TOK_B + jnp.arange(TOK_B * TOP, dtype=jnp.int32)[None, :] // TOP).astype(jnp.int32)
    table_token = jnp.zeros((EXPERTS, block_count * CAP), jnp.int32).at[flattened_expert_list.reshape(-1), place.reshape(-1)].set(token_ids.reshape(-1))
    table_weight = jnp.zeros((EXPERTS, block_count * CAP), jnp.float32).at[flattened_expert_list.reshape(-1), place.reshape(-1)].set(route_weights.astype(jnp.float32).reshape(-1))
    unit_width = FF // GROUPS

    def one_expert(carry, operands):
        gate_e, up_e, down_e, token_list, weight_list = operands
        picked = jnp.take(normed, token_list, axis=0)
        gate_val = jnp.dot(picked, gate_e, preferred_element_type=jnp.float32)
        up_val = jnp.dot(picked, up_e, preferred_element_type=jnp.float32)
        hidden = (jax.nn.silu(gate_val) * up_val).astype(jnp.bfloat16)
        expert_sum = jnp.zeros((token_list.shape[0], D), jnp.float32)
        for group_no in range(GROUPS):
            lower = group_no * unit_width
            partial_sum = jnp.dot(hidden[:, lower:lower + unit_width], down_e[lower:lower + unit_width], preferred_element_type=jnp.float32)
            expert_sum = expert_sum + to_bf_and_back(partial_sum)
        result = to_bf_and_back(expert_sum)
        carry = carry.at[token_list].add(weight_list[:, None] * result)
        return (carry, None)
    moe_total = lax.scan(one_expert, jnp.zeros((TOKENS_B, D), jnp.float32), (gate_weight, up_weight, down_weight, table_token, table_weight))[0]
    moe_out = moe_total.astype(jnp.bfloat16)
    return (mixed, moe_out)
```

```python
import functools
import math

import jax
import jax.numpy as jnp
from jax import lax
from jax.experimental import pallas as pl
from jax.experimental.pallas import tpu as pltpu
from jax.sharding import PartitionSpec as P


F32 = jnp.float32
BF16 = jnp.bfloat16
VMEM = pl.BlockSpec(memory_space=pltpu.VMEM)
SMEM = pl.BlockSpec(memory_space=pltpu.SMEM)
VMEM_LIMIT = 56 * 1024 * 1024


def swap(value, axis, distance):
    count = lax.axis_size(axis)
    return lax.ppermute(value, axis, [(i, i ^ distance) for i in range(count)])


def dot(a, b):
    return jnp.dot(a, b, preferred_element_type=F32)


def dispatch_kernel(capacity, me_ref, tokens_ref, gain_ref, routes_ref, *out_refs):
    place_ref, chunk_refs = out_refs[0], out_refs[1:]
    chunk_rows = chunk_refs[0].shape[0]
    expert_total = len(chunk_refs) * chunk_rows // capacity
    tokens = tokens_ref[...].astype(F32)
    rows, top = routes_ref.shape
    scale = lax.rsqrt(jnp.mean(tokens * tokens, axis=1, keepdims=True) + 1e-06)
    normed = (tokens * scale * gain_ref[...].astype(F32)).astype(BF16)
    chunk_of = jnp.bitwise_xor(routes_ref[...], me_ref[0])
    lanes = lax.broadcasted_iota(jnp.int32, (rows, expert_total), 1)
    named = [(chunk_of[:, k : k + 1] == lanes).astype(F32) for k in range(top)]
    every = functools.reduce(jnp.add, named)
    below = (
        lax.broadcasted_iota(jnp.int32, (rows, rows), 0)
        > lax.broadcasted_iota(jnp.int32, (rows, rows), 1)
    ).astype(F32)
    earlier = dot(below.astype(BF16), every.astype(BF16))
    slots = lax.broadcasted_iota(jnp.int32, (rows, expert_total * capacity), 1)
    table = jnp.zeros((rows, expert_total * capacity), F32)
    for k in range(top):
        slot = jnp.sum(earlier * named[k], axis=1, keepdims=True).astype(jnp.int32)
        place = chunk_of[:, k : k + 1] * capacity + slot
        place_ref[:, k : k + 1] = place
        table = table + (slots == place).astype(F32)
    table = table.astype(BF16)
    for chunk, ref in enumerate(chunk_refs):
        part = table[:, chunk * chunk_rows : (chunk + 1) * chunk_rows]
        ref[...] = lax.dot_general(
            part, normed, (((0,), (0,)), ((), ())), preferred_element_type=F32
        ).astype(BF16)


def dispatch(me, tokens, gain, routes, expert_total, capacity, chunk_total):
    rows, width = tokens.shape
    chunk_rows = expert_total * capacity // chunk_total
    return pl.pallas_call(
        functools.partial(dispatch_kernel, capacity),
        out_shape=[jax.ShapeDtypeStruct(routes.shape, jnp.int32)]
        + [jax.ShapeDtypeStruct((chunk_rows, width), BF16)] * chunk_total,
        in_specs=[SMEM, VMEM, VMEM, VMEM],
        out_specs=[VMEM] * (chunk_total + 1),
        compiler_params=pltpu.CompilerParams(vmem_limit_bytes=VMEM_LIMIT),
        name="dispatch",
    )(me, tokens, gain.reshape(1, width), routes)


def attend_kernel(blocks, me_ref, query_ref, kv_ref, weight_ref, keep_ref, send_ref, attended_ref):
    row_total, flat = query_ref.shape
    head_dim = kv_ref.shape[2] // 2
    heads = flat // head_dim
    span = row_total
    me, me_tp = me_ref[0], me_ref[1]
    score_scale = 1.0 / math.sqrt(head_dim)
    queries = jnp.concatenate(
        [query_ref[:, h * head_dim : (h + 1) * head_dim] for h in range(heads)], axis=0
    )
    after_mask = (
        lax.broadcasted_iota(jnp.int32, (span, span), 0)
        > lax.broadcasted_iota(jnp.int32, (span, span), 1)
    ).astype(F32).astype(BF16)
    row_pos = lax.broadcasted_iota(jnp.int32, (row_total, span), 0)
    col_pos = lax.broadcasted_iota(jnp.int32, (row_total, span), 1)
    earlier_one = (col_pos < row_pos).astype(F32)
    earlier = jnp.concatenate([earlier_one] * heads, axis=0)

    def block(owner, mask, accum, carried):
        offset = jnp.bitwise_xor(owner, me)
        at, size = 0, kv_ref.shape[0]
        for bit in range(size.bit_length() - 1):
            at = at * 2 + jnp.bitwise_and(jnp.right_shift(offset, bit), 1)
        key_rows = kv_ref[at, :span, :head_dim]
        value_rows = kv_ref[at, :span, head_dim:]
        bias = kv_ref[at, span : span + heads, :span].astype(F32)
        scores = lax.dot_general(
            queries, key_rows, (((1,), (1,)), ((), ())), preferred_element_type=F32
        ) * score_scale
        scores = jnp.concatenate(
            [
                scores[h * row_total : (h + 1) * row_total] + bias[h : h + 1, :]
                for h in range(heads)
            ],
            axis=0,
        )
        small = jnp.exp(-jnp.abs(scores))
        soft = jnp.where(small < 1e-3, small * (1.0 - 0.5 * small), jnp.log(1.0 + small))
        drop = jnp.maximum(scores, 0.0) + soft
        if mask is not None:
            drop = drop * mask
        high = drop.astype(BF16)
        low = (drop - high.astype(F32)).astype(BF16)
        after = dot(high, after_mask) + dot(low, after_mask)
        weights = jnp.exp((jnp.minimum(scores, 0.0) - soft) - after - carried)
        if mask is not None:
            weights = weights * mask
        accum = accum + dot(weights.astype(BF16), value_rows)
        carried = carried + after[:, 0:1] + drop[:, 0:1]
        return accum, carried

    state = block(
        me,
        earlier,
        jnp.zeros((heads * row_total, head_dim), F32),
        jnp.zeros((heads * row_total, 1), F32),
    )
    accum, _ = lax.fori_loop(
        0, me, lambda step, state: block(me - 1 - step, None, *state), state
    )
    for h in range(heads):
        attended_ref[:, h * head_dim : (h + 1) * head_dim] = accum[
            h * row_total : (h + 1) * row_total
        ]
    own = row_total // blocks
    places = {True: 0, False: 0}
    for number in range(blocks):
        begin = pl.multiple_of(jnp.bitwise_xor(me_tp, number) * own, own)
        rows = attended_ref[pl.ds(begin, own), :].astype(BF16)
        partial = dot(rows, weight_ref[...]).astype(BF16)
        keep = number % 2 == 0
        ref = keep_ref if keep else send_ref
        ref[places[keep] : places[keep] + own, :] = partial
        places[keep] += own


def attend(me, queries, kv, out_weight, blocks):
    rows, heads, head_dim = queries.shape
    width = out_weight.shape[1]
    half = jax.ShapeDtypeStruct((rows // 2, width), BF16)
    return pl.pallas_call(
        functools.partial(attend_kernel, blocks),
        out_shape=[half, half],
        in_specs=[SMEM, VMEM, VMEM, VMEM],
        out_specs=[VMEM, VMEM],
        scratch_shapes=[pltpu.VMEM((rows, heads * head_dim), F32)],
        compiler_params=pltpu.CompilerParams(vmem_limit_bytes=VMEM_LIMIT),
        name="attend",
    )(me, queries.reshape(rows, heads * head_dim), kv, out_weight)


def expert_kernel(near, *refs):
    row_refs, (gate_ref, up_ref, down_ref), (keep_ref, send_ref) = refs[:-5], refs[-5:-2], refs[-2:]

    def partial(refs_of):
        rows = jnp.concatenate([ref[...] for ref in refs_of], axis=0)
        gate = dot(rows, gate_ref[...])
        up = dot(rows, up_ref[...])
        hidden = (gate / (1.0 + jnp.exp(-gate)) * up).astype(BF16)
        return dot(hidden, down_ref[...]).astype(BF16)

    send_ref[...] = partial(row_refs[near:])
    keep_ref[...] = partial(row_refs[:near])


def experts(near_rows, far_rows, gate_cols, up_cols, down_rows):
    rows = near_rows + far_rows
    half = jax.ShapeDtypeStruct(
        (sum(piece.shape[0] for piece in near_rows), down_rows.shape[1]), BF16
    )
    return pl.pallas_call(
        functools.partial(expert_kernel, len(near_rows)),
        out_shape=[half, half],
        in_specs=[VMEM] * (len(rows) + 3),
        out_specs=[VMEM, VMEM],
        compiler_params=pltpu.CompilerParams(vmem_limit_bytes=VMEM_LIMIT),
        name="experts",
    )(*rows, gate_cols, up_cols, down_rows)


def combine_kernel(place_ref, share_ref, *refs):
    chunk_refs, out_ref, gathered_ref = refs[:-2], refs[-2], refs[-1]
    capacity = chunk_refs[0].shape[0]
    rows, top = place_ref.shape
    total = gathered_ref.shape[0]
    for chunk, ref in enumerate(chunk_refs):
        gathered_ref[chunk * capacity : (chunk + 1) * capacity, :] = ref[...].astype(F32)
    gathered = gathered_ref[...].astype(BF16)
    slots = lax.broadcasted_iota(jnp.int32, (rows, total), 1)
    mixed = jnp.zeros(out_ref.shape, F32)
    for k in range(top):
        table = (slots == place_ref[:, k : k + 1]).astype(F32).astype(BF16)
        mixed = mixed + dot(table, gathered) * share_ref[:, k : k + 1]
    out_ref[...] = mixed.astype(BF16)


def combine(place, shares, chunks):
    rows = place.shape[0]
    capacity, width = chunks[0].shape
    return pl.pallas_call(
        combine_kernel,
        out_shape=jax.ShapeDtypeStruct((rows, width), BF16),
        in_specs=[VMEM] * (len(chunks) + 2),
        out_specs=VMEM,
        scratch_shapes=[pltpu.VMEM((len(chunks) * capacity, width), F32)],
        compiler_params=pltpu.CompilerParams(vmem_limit_bytes=VMEM_LIMIT),
        name="combine",
    )(place, shares, *chunks)


def add(a, b):
    return (a.astype(F32) + b.astype(F32)).astype(BF16)


def gather_blocks(block, axis):
    stacked = block[None]
    distance = lax.axis_size(axis) // 2
    while distance:
        stacked = jnp.concatenate([stacked, swap(stacked, axis, distance)], axis=0)
        distance //= 2
    return stacked


def body(
    queries,
    keys,
    values,
    key_bias,
    out_weight,
    tokens_b,
    moe_gain,
    gate_weight,
    up_weight,
    down_weight,
    routes,
    route_weights,
):
    tok_rows, local_heads, head_dim = queries.shape
    ep_count, tp_count = lax.axis_size("ep"), lax.axis_size("tp")
    me = jnp.stack([lax.axis_index("ep"), lax.axis_index("tp")]).astype(jnp.int32)
    tok_b, model_width = tokens_b.shape
    top_count = routes.shape[1]
    capacity = max(2, 3 * top_count * tok_b // (2 * ep_count))

    kv_width = 2 * head_dim
    bias_rows = jnp.pad(
        jnp.transpose(key_bias), ((0, 16 - local_heads), (0, kv_width - tok_rows))
    )
    own_kv = jnp.concatenate(
        [
            jnp.concatenate([keys[:, 0], values[:, 0]], axis=1),
            bias_rows,
        ],
        axis=0,
    )
    kv = gather_blocks(own_kv, "ep")

    paired = ep_count <= 8
    chunk_total = ep_count if paired else 1
    chunk_rows = ep_count * capacity // chunk_total

    def exchange(piece, chunk):
        if not paired:
            piece = piece.reshape(ep_count, capacity, model_width)
            piece = lax.all_to_all(piece, "ep", split_axis=0, concat_axis=0, tiled=True)
            return piece.reshape(chunk_rows, model_width)
        return piece if chunk == 0 else swap(piece, "ep", chunk)

    first = me if paired else jnp.zeros_like(me)
    place, *chunks = dispatch(
        first, tokens_b, moe_gain, routes, ep_count, capacity, chunk_total
    )
    tp_steps = []
    distance = tp_count // 2
    while distance:
        tp_steps.append(distance)
        distance //= 2

    group_count = min(4, chunk_total)
    group_size = chunk_total // group_count
    returned = []
    for group in range(group_count):
        near, far = [], []
        for chunk in range(group * group_size, (group + 1) * group_size):
            have = [exchange(chunks[chunk], chunk)]
            for distance in tp_steps[:-1]:
                have = have + [swap(piece, "tp", distance) for piece in have]
            near += have
            far += [swap(piece, "tp", tp_steps[-1]) for piece in have]
        keep, send = experts(near, far, gate_weight[0], up_weight[0], down_weight[0])
        total = add(keep, swap(send, "tp", tp_steps[-1]))
        total = total.reshape(group_size, tp_count // 2, chunk_rows, model_width)
        for number in range(group_size):
            parts = [total[number, i] for i in range(tp_count // 2)]
            for distance in reversed(tp_steps[:-1]):
                half = len(parts) // 2
                parts = [add(a, swap(b, "tp", distance)) for a, b in zip(parts[:half], parts[half:])]
            returned.append(exchange(parts[0], group * group_size + number))
    moe_out = combine(place, route_weights, returned)

    keep, send = attend(me, queries, kv, out_weight, tp_count)
    total = add(keep, swap(send, "tp", 1)).reshape(tp_count // 2, -1, model_width)
    parts = [total[i] for i in range(tp_count // 2)]
    for distance in reversed(tp_steps[:-1]):
        half = len(parts) // 2
        parts = [add(a, swap(b, "tp", distance)) for a, b in zip(parts[:half], parts[half:])]
    return (parts[0], moe_out)


def solution(mesh):
    in_specs = (
        P("ep", "tp", None),
        P("ep", "tp", None),
        P("ep", "tp", None),
        P("ep", "tp"),
        P("tp", None),
        P(("ep", "tp"), None),
        P(),
        P("ep", None, "tp"),
        P("ep", None, "tp"),
        P("ep", "tp", None),
        P(("ep", "tp"), None),
        P(("ep", "tp"), None),
    )
    out_specs = (P(("ep", "tp"), None), P(("ep", "tp"), None))
    return jax.shard_map(body, mesh=mesh, in_specs=in_specs, out_specs=out_specs, check_vma=False)
```
